32 devices in a mesh: grp: 2 (over y), fs: 4 (over z), tp: 4 (over x, core).
Axes of the slice: x: 2, y: 2, z: 4, core: 2. Of those that a mesh axis runs over, the one named last changes fastest.
Arguments:
- tokens: bfloat16 [8192, 2048], P(('grp', 'fs')), parts along dimension 0, may hold values from -6 to 6
- mixer_gain: float32 [2048], replicated, may hold values from 0.1 to 1.9
- outer_weight: float32 [2048, 2048], P('fs', 'tp'), may hold values from -0.125 to 0.125
- inner_weight: float32 [2048, 2048], P('fs', 'tp'), may hold values from -0.125 to 0.125
- value_weight: float32 [2048, 2048], P('fs', 'tp'), may hold values from -0.125 to 0.125
- filter_taps: float32 [3, 2048], P(None, 'tp'), may hold values from -3.5 to 3.5
- mixer_weight: float32 [2048, 2048], P('tp', 'fs'), may hold values from -0.125 to 0.125
- outer_scale: float32 [4, 512], P('tp', 'fs'), may hold values from 0.5 to 2
- inner_scale: float32 [4, 512], P('tp', 'fs'), may hold values from 0.5 to 2
- value_scale: float32 [4, 512], P('tp', 'fs'), may hold values from 0.5 to 2
- mixer_scale: float32 [1, 2048], P(None, 'fs'), may hold values from 0.5 to 2
Outputs:
- layer_out: bfloat16 [8192, 2048], P(('grp', 'fs', 'tp')), parts along dimension 0
The draws below stay inside these ranges and needn't reach their ends.
There are 2 independent parts, one for each index of `grp`. The reference program is written for one: setup_inputs(seed, part) draws one part's arguments, and reference() takes and returns one part's arrays. A program takes and returns all parts, laid end to end along the dimension named above; an argument that names none is the same for every part. Nothing has to cross between parts.
All inputs are finite; a program needn't handle non-finite values.
Results may differ from the reference program's by a relative error of at most 0.014.
Values may be sent and summed in bfloat16 or wider, within the bound.
No kernel may reach another device: no remote copies, remote signals or barrier semaphores. Data moves between devices by JAX's collectives and lax.ppermute only.
A program may use at most 64 MiB of HBM per device.

```python
import math
import jax
import jax.numpy as jnp
from jax import lax

D = 2048
DC = 2048
SEQ_LEN = 1024
TOKENS = 4096
N_FS = 4
N_TP = 4


def levels(key, dims, shards, smallest, top_value):
    factor_of = 1.0
    for axis_at, blocks in shards:
        heights = jax.random.uniform(jax.random.fold_in(jax.random.fold_in(key, 6), axis_at), (blocks,), jnp.float32, smallest / len(shards), top_value / len(shards))
        factor_of = factor_of * jnp.repeat(jnp.exp(heights), dims[axis_at] // blocks).reshape((-1,) + (1,) * (len(dims) - 1 - axis_at))
    return factor_of


def centred(stream_key, dims, scale, reach, cuts=(), held_as=jnp.bfloat16):
    drawn = scale * jax.random.normal(stream_key, dims, jnp.float32)
    if cuts:
        drawn = drawn * levels(stream_key, dims, cuts, -0.22, 0.18)
    return jnp.clip(drawn, -reach, reach).astype(held_as)


def setup_inputs(seed: int = 0, part: int = 0) -> dict:
    streams_of = jax.random.split(jax.random.key(seed), 12)
    own_keys = jax.random.split(jax.random.fold_in(streams_of[11], part), 12)
    tokens = centred(own_keys[0], (TOKENS, D), 1.0, 6.0, ((0, 4),))
    mixer_gain = jnp.clip(1.0 + 0.18 * jax.random.normal(streams_of[1], (D,), jnp.float32), 0.1, 1.9)
    outer_weight = centred(streams_of[2], (D, DC), D ** -0.5, 0.125, ((0, 4), (1, 4)), jnp.float32)
    inner_weight = centred(streams_of[3], (D, DC), D ** -0.5, 0.125, ((0, 4), (1, 4)), jnp.float32)
    value_weight = centred(streams_of[4], (D, DC), D ** -0.5, 0.125, ((0, 4), (1, 4)), jnp.float32)
    filter_taps = centred(streams_of[5], (3, DC), 3 ** -0.5, 3.5, ((1, 4),), jnp.float32)
    mixer_weight = centred(streams_of[6], (DC, D), DC ** -0.5, 0.125, ((0, 4), (1, 4)), jnp.float32)
    outer_scale = jnp.clip(jnp.exp(math.log(2.0) - 1.3862944 * jax.random.uniform(streams_of[7], (N_TP, DC // N_TP), jnp.float32) ** levels(streams_of[7], (N_TP, DC // N_TP), ((0, 4), (1, 4)), -0.2, 0.2)), 0.5, 2.0)
    inner_scale = jnp.clip(jnp.exp(math.log(2.0) - 1.3862944 * jax.random.uniform(streams_of[8], (N_TP, DC // N_TP), jnp.float32) ** levels(streams_of[8], (N_TP, DC // N_TP), ((0, 4), (1, 4)), -0.2, 0.2)), 0.5, 2.0)
    value_scale = jnp.clip(jnp.exp(math.log(2.0) - 1.3862944 * jax.random.uniform(streams_of[9], (N_TP, DC // N_TP), jnp.float32) ** levels(streams_of[9], (N_TP, DC // N_TP), ((0, 4), (1, 4)), -0.2, 0.2)), 0.5, 2.0)
    mixer_scale = jnp.clip(jnp.exp(math.log(2.0) - 1.3862944 * jax.random.uniform(streams_of[10], (1, D), jnp.float32) ** levels(streams_of[10], (1, D), ((1, 4),), -0.2, 0.2)), 0.5, 2.0)
    return dict(tokens=tokens, mixer_gain=mixer_gain, outer_weight=outer_weight, inner_weight=inner_weight, value_weight=value_weight, filter_taps=filter_taps, mixer_weight=mixer_weight, outer_scale=outer_scale, inner_scale=inner_scale, value_scale=value_scale, mixer_scale=mixer_scale)


EPS = 1e-06

def normed(rows, gain):
    values = rows.astype(jnp.float32)
    inverse = lax.rsqrt(lax.optimization_barrier(jnp.mean(values * values, axis=-1, keepdims=True)) + EPS)
    return (values * inverse * gain).astype(jnp.bfloat16)

def project(left, weight, scale):
    return jnp.dot(left, weight.astype(jnp.bfloat16), preferred_element_type=jnp.float32) * scale.reshape(-1)

def rounded(values):
    return lax.optimization_barrier(values.astype(jnp.bfloat16)).astype(jnp.float32)

def summed_blocks(hidden, weight, scale):
    width = hidden.shape[1] // N_TP
    total = jnp.zeros((hidden.shape[0], weight.shape[1]), jnp.float32)
    for index in range(N_TP):
        part = project(hidden[:, index * width:(index + 1) * width], weight[index * width:(index + 1) * width], scale)
        total = total + rounded(part)
    return total

def reference(tokens, mixer_gain, outer_weight, inner_weight, value_weight, filter_taps, mixer_weight, outer_scale, inner_scale, value_scale, mixer_scale):
    normal_rows = normed(tokens, mixer_gain)
    outer = rounded(project(normal_rows, outer_weight, outer_scale))
    inner = rounded(project(normal_rows, inner_weight, inner_scale))
    value = rounded(project(normal_rows, value_weight, value_scale))
    product = (inner * value).reshape(N_FS, SEQ_LEN, DC)
    padded = jnp.pad(product, ((0, 0), (2, 0), (0, 0)))
    filtered = filter_taps[0] * padded[:, 0:SEQ_LEN] + filter_taps[1] * padded[:, 1:SEQ_LEN + 1] + filter_taps[2] * padded[:, 2:]
    gated = (outer * filtered.reshape(TOKENS, DC)).astype(jnp.bfloat16)
    return summed_blocks(gated, mixer_weight, mixer_scale).astype(jnp.bfloat16)
```

```python
import jax
import jax.numpy as jnp
from jax import lax
from jax.experimental import pallas as pl
from jax.experimental.pallas import tpu as pltpu
from jax.sharding import PartitionSpec as P

EPS = 1e-06
F32 = jnp.float32
BF16 = jnp.bfloat16
LANES = 128


def normed(rows, gain):
    values = rows.astype(F32)
    inverse = lax.rsqrt(jnp.mean(values * values, axis=-1, keepdims=True) + EPS)
    return (values * inverse * gain).astype(BF16)


def rounded(values):
    return lax.optimization_barrier(values.astype(BF16)).astype(F32)


def plain_device(
    tokens,
    mixer_gain,
    outer_weight,
    inner_weight,
    value_weight,
    filter_taps,
    mixer_weight,
    outer_scale,
    inner_scale,
    value_scale,
    mixer_scale,
):
    scales = (outer_scale, inner_scale, value_scale, mixer_scale)
    outer_col, inner_col, value_col, mixer_col = [
        lax.all_gather(piece, "fs", axis=1, tiled=True).reshape(-1) for piece in scales
    ]
    seq_rows = tokens.shape[0]
    normal_rows = normed(tokens, mixer_gain)

    def project(weight, col):
        full = lax.all_gather(weight.astype(BF16), "fs", axis=0, tiled=True)
        return rounded(jnp.dot(normal_rows, full, preferred_element_type=F32) * col)

    outer = project(outer_weight, outer_col)
    inner = project(inner_weight, inner_col)
    value = project(value_weight, value_col)
    padded = jnp.pad(inner * value, ((2, 0), (0, 0)))
    filtered = (
        filter_taps[0] * padded[0:seq_rows]
        + filter_taps[1] * padded[1 : seq_rows + 1]
        + filter_taps[2] * padded[2:]
    )
    gated = (outer * filtered).astype(BF16)
    mixer_full = lax.all_gather(mixer_weight.astype(BF16), "fs", axis=1, tiled=True)
    part = (jnp.dot(gated, mixer_full, preferred_element_type=F32) * mixer_col).astype(BF16)
    return lax.psum_scatter(part, "tp", scatter_dimension=0, tiled=True)


def ring_order(count):
    return list(range(0, count, 2)) + [i for i in range(count - 1, 0, -1) if i % 2]


def source_at(count, step):
    me = lax.axis_index("fs")
    half_up = (count + 1) // 2
    place = jnp.where(me % 2 == 0, me // 2, count - 1 - me // 2)
    place = jnp.where(place >= step, place - step, place - step + count)
    return jnp.where(place < half_up, 2 * place, 2 * (count - 1 - place) + 1)


def whole():
    return pl.BlockSpec(memory_space=pltpu.VMEM)


def anywhere():
    return pl.BlockSpec(memory_space=pl.ANY)


def norm_kernel(tok_ref, gain_ref, out_ref):
    values = tok_ref[...].astype(F32)
    inverse = lax.rsqrt(jnp.mean(values * values, axis=-1, keepdims=True) + EPS)
    out_ref[...] = (values * inverse * gain_ref[...]).astype(BF16)


def norm_call(tokens, gain):
    rows, width = tokens.shape
    block = rows // 8
    return pl.pallas_call(
        norm_kernel,
        out_shape=jax.ShapeDtypeStruct((rows, width), BF16),
        grid=(rows // block,),
        in_specs=[
            pl.BlockSpec((block, width), lambda i: (i, 0)),
            pl.BlockSpec((1, width), lambda i: (0, 0)),
        ],
        out_specs=pl.BlockSpec((block, width), lambda i: (i, 0)),
        cost_estimate=pl.CostEstimate(
            flops=8 * rows * width, bytes_accessed=4 * rows * width, transcendentals=rows
        ),
        name="norm",
    )(tokens, gain.reshape(1, width))


def load_weight(count, own_ref, piece_refs, full, sem):
    me = lax.axis_index("fs")
    grp = lax.axis_index("grp")
    depth = own_ref.shape[0]
    half = depth // 2
    copies = []
    for step in range(1, count):
        base = source_at(count, step) * depth
        for side in range(2):
            which = grp if side == 0 else 1 - grp
            at = pl.multiple_of(base + which * half, half)
            index = 2 * (step - 1) + side
            copies.append(
                pltpu.make_async_copy(piece_refs[index], full.at[pl.ds(at, half)], sem.at[index])
            )
    for copy in copies:
        copy.start()
    full[pl.ds(pl.multiple_of(me * depth, depth), depth)] = own_ref[...].astype(BF16)
    for copy in copies:
        copy.wait()


def column_scale(scale_ref, slot, width):
    count = scale_ref.shape[0]
    each = width // count
    return jnp.concatenate(
        [scale_ref[i : i + 1, slot * each : (slot + 1) * each] for i in range(count)], axis=1
    )


def project_kernel(count, slot, x_ref, scale_ref, own_ref, *rest):
    pieces = 2 * (count - 1)
    piece_refs, (out_ref, full, sem) = rest[:pieces], rest[pieces:]

    @pl.when(pl.program_id(0) == 0)
    def _():
        load_weight(count, own_ref, piece_refs, full, sem)

    scale = column_scale(scale_ref, slot, out_ref.shape[1])
    acc = jnp.dot(x_ref[...], full[...], preferred_element_type=F32)
    out_ref[...] = (acc * scale).astype(BF16)


def gate_kernel(count, slot, x_ref, outer_ref, inner_ref, taps_ref, scale_ref, own_ref, *rest):
    pieces = 2 * (count - 1)
    piece_refs, (out_ref, full, carry, sem) = rest[:pieces], rest[pieces:]
    rows = x_ref.shape[0]

    @pl.when(pl.program_id(0) == 0)
    def _():
        load_weight(count, own_ref, piece_refs, full, sem)
        carry[...] = jnp.zeros_like(carry)

    scale = column_scale(scale_ref, slot, out_ref.shape[1])
    acc = jnp.dot(x_ref[...], full[...], preferred_element_type=F32)
    value = (acc * scale).astype(BF16).astype(F32)
    product = inner_ref[...].astype(F32) * value
    tail = carry.shape[0]
    padded = jnp.concatenate([carry[...], product], axis=0)
    carry[...] = product[rows - tail :]
    filtered = (
        taps_ref[0:1] * padded[tail - 2 : tail - 2 + rows]
        + taps_ref[1:2] * padded[tail - 1 : tail - 1 + rows]
        + taps_ref[2:3] * product
    )
    out_ref[...] = (outer_ref[...].astype(F32) * filtered).astype(BF16)


def project_call(count, slot, x, scales, own, pieces, extra=(), kernel=project_kernel, name="project"):
    rows, width = x.shape
    cols = own.shape[1]
    block = rows // 4
    scratch = [pltpu.VMEM((width, cols), BF16)]
    if extra:
        scratch.append(pltpu.VMEM((8, cols), F32))
    scratch.append(pltpu.SemaphoreType.DMA((len(pieces),)))
    row_block = pl.BlockSpec((block, cols), lambda i: (i, 0))
    extra_specs = [row_block, row_block, whole()] if extra else []
    return pl.pallas_call(
        lambda *refs: kernel(count, slot, *refs),
        out_shape=jax.ShapeDtypeStruct((rows, cols), BF16),
        grid=(rows // block,),
        in_specs=[pl.BlockSpec((block, width), lambda i: (i, 0))]
        + extra_specs
        + [whole(), whole()]
        + [anywhere()] * len(pieces),
        out_specs=row_block,
        scratch_shapes=scratch,
        cost_estimate=pl.CostEstimate(
            flops=2 * rows * width * cols,
            bytes_accessed=2 * (rows * width + width * cols + 2 * rows * cols),
            transcendentals=0,
        ),
        name=name,
    )(x, *extra, scales, own, *pieces)


def part_kernel(count, step, lead, g_ref, scale_ref, *rest):
    weight_refs, (keep_ref, give_ref) = rest[:-2], rest[-2:]
    grp = lax.axis_index("grp")
    core = lax.axis_index("tp") % 2
    chips, block, cols = keep_ref.shape
    scale = scale_ref[pl.ds(source_at(count, step), 1), lead:]
    if len(weight_refs) == 1:
        weights = [(0, weight_refs[0].shape[0], weight_refs[0][...].astype(BF16))]
    else:
        half = weight_refs[0].shape[0]
        weights = [(grp * half, half, weight_refs[0][...]), ((1 - grp) * half, half, weight_refs[1][...])]
    for chip in range(chips):
        for side, out_ref in ((core, keep_ref), (1 - core, give_ref)):
            rows = pl.ds(pl.multiple_of((2 * chip + side) * block, block), block)
            acc = None
            for start, size, weight in weights:
                if isinstance(start, int):
                    left = g_ref[rows, start : start + size]
                else:
                    left = g_ref[rows, pl.ds(pl.multiple_of(start, size), size)]
                term = jnp.dot(left, weight, preferred_element_type=F32)
                acc = term if acc is None else acc + term
            out_ref[chip] = (acc * scale).astype(BF16)


def part_call(count, step, lead, chips, gated, scales, weights):
    rows, depth = gated.shape
    cols = weights[0].shape[1]
    block = rows // (2 * chips)
    shape = jax.ShapeDtypeStruct((chips, block, cols), BF16)
    return pl.pallas_call(
        lambda *refs: part_kernel(count, step, lead, *refs),
        out_shape=(shape, shape),
        in_specs=[whole()] * (2 + len(weights)),
        out_specs=(whole(), whole()),
        cost_estimate=pl.CostEstimate(
            flops=2 * rows * depth * cols,
            bytes_accessed=2 * (rows * depth + depth * cols + rows * cols),
            transcendentals=0,
        ),
        name="part",
    )(gated, scales, *weights)


def pair_kernel(keep_ref, got_ref, mine_ref, *send_refs):
    chips = keep_ref.shape[0]
    chip = lax.axis_index("tp") // 2

    def total(index):
        return (keep_ref[index].astype(F32) + got_ref[index].astype(F32)).astype(BF16)

    mine_ref[...] = total(chip)
    for away, send_ref in enumerate(send_refs, 1):
        send_ref[...] = total((chip + away) % chips)


def pair_call(keep, got):
    chips, block, cols = keep.shape
    shape = jax.ShapeDtypeStruct((block, cols), BF16)
    return pl.pallas_call(
        pair_kernel,
        out_shape=(shape,) * chips,
        in_specs=[whole()] * 2,
        out_specs=(whole(),) * chips,
        cost_estimate=pl.CostEstimate(
            flops=chips * block * cols, bytes_accessed=6 * chips * block * cols, transcendentals=0
        ),
        name="pair",
    )(keep, got)


def final_kernel(count, terms, *refs):
    ins, out_ref = refs[:-1], refs[-1]
    cols = out_ref.shape[1] // count
    for step in range(count):
        acc = ins[step * terms][...].astype(F32)
        for term in range(1, terms):
            acc = acc + ins[step * terms + term][...].astype(F32)
        at = pl.multiple_of(source_at(count, step) * cols, cols)
        out_ref[:, pl.ds(at, cols)] = acc.astype(BF16)


def final_call(count, terms, arrays):
    block, cols = arrays[0].shape
    return pl.pallas_call(
        lambda *refs: final_kernel(count, terms, *refs),
        out_shape=jax.ShapeDtypeStruct((block, count * cols), BF16),
        in_specs=[whole()] * len(arrays),
        out_specs=whole(),
        cost_estimate=pl.CostEstimate(
            flops=count * block * cols,
            bytes_accessed=2 * (terms + 1) * count * block * cols,
            transcendentals=0,
        ),
        name="final",
    )(*arrays)


def ring_device(
    count,
    chips,
    tokens,
    mixer_gain,
    outer_weight,
    inner_weight,
    value_weight,
    filter_taps,
    mixer_weight,
    outer_scale,
    inner_scale,
    value_scale,
    mixer_scale,
):
    order = ring_order(count)
    ring = [(order[i], order[(i + 1) % count]) for i in range(count)]
    swap_cores = [(2 * c + k, 2 * c + 1 - k) for c in range(chips) for k in range(2)]
    grp = lax.axis_index("grp")

    def halves(weight):
        half = weight.shape[0] // 2
        return lax.dynamic_slice_in_dim(weight, grp * half, half, 0).astype(BF16)

    def travel(weight):
        piece = halves(weight)
        pieces = []
        for _ in range(count - 1):
            piece = lax.ppermute(piece, "fs", ring)
            pieces += [piece, lax.ppermute(piece, "grp", [(0, 1), (1, 0)])]
        return pieces

    outer_pieces = travel(outer_weight)
    inner_pieces = travel(inner_weight)
    value_pieces = travel(value_weight)
    mixer_pieces = travel(mixer_weight)

    packed = jnp.concatenate([outer_scale, inner_scale, value_scale, mixer_scale], axis=1)
    scales = lax.all_gather(packed, "fs", axis=0, tiled=True)
    lead = 3 * outer_scale.shape[1]

    x = norm_call(tokens, mixer_gain)
    outer = project_call(count, 0, x, scales, outer_weight, outer_pieces)
    inner = project_call(count, 1, x, scales, inner_weight, inner_pieces)
    gated = project_call(
        count,
        2,
        x,
        scales,
        value_weight,
        value_pieces,
        (outer, inner, filter_taps),
        gate_kernel,
        "gate",
    )
    finals = []
    for step in range(count):
        weights = (
            [mixer_weight] if step == 0 else mixer_pieces[2 * (step - 1) : 2 * step]
        )
        keep, give = part_call(count, step, lead, chips, gated, scales, weights)
        got = lax.ppermute(give, "tp", swap_cores)
        mine, *sends = pair_call(keep, got)
        finals.append(mine)
        for away, send in enumerate(sends, 1):
            move = [
                (2 * c + k, 2 * ((c + away) % chips) + k) for c in range(chips) for k in range(2)
            ]
            finals.append(lax.ppermute(send, "tp", move))
    return final_call(count, chips, finals)


def solution(mesh):
    in_specs = (
        P(("grp", "fs"), None),
        P(),
        P("fs", "tp"),
        P("fs", "tp"),
        P("fs", "tp"),
        P(None, "tp"),
        P("tp", "fs"),
        P("tp", "fs"),
        P("tp", "fs"),
        P("tp", "fs"),
        P(None, "fs"),
    )
    out_specs = P(("grp", "fs", "tp"), None)
    count, groups, blocks = mesh.shape["fs"], mesh.shape["grp"], mesh.shape["tp"]

    def step(*args):
        depth, width = args[2].shape[0] // count, args[2].shape[1] // blocks
        fits = depth % (2 * LANES) == 0 and width % (count * LANES) == 0
        if groups == 2 and blocks % 2 == 0 and fits:
            body = lambda *shards: ring_device(count, blocks // 2, *shards)
        else:
            body = plain_device
        return jax.shard_map(
            body, mesh=mesh, in_specs=in_specs, out_specs=out_specs, check_vma=False
        )(*args)

    return step
```
